32 devices in a mesh: grp: 2 (over y), ep: 4 (over z), tp: 4 (over x, core).
Axes of the slice: x: 2, y: 2, z: 4, core: 2. Of those that a mesh axis runs over, the one named last changes fastest.
Arguments:
- mixer_input: bfloat16 [4096, 2048], P(('grp', 'ep', 'tp')), parts along dimension 0, may hold values from -8 to 8
- forget_cumsum: float32 [8, 4096], P('tp', 'grp'), parts along dimension 1, may hold values from -259 to 0, as said below
- mixer_gain: float32 [2048], replicated, may hold values from 0.1 to 1.9
- query_weight: bfloat16 [2048, 1024], P(None, 'tp'), may hold values from -6 to 6
- key_weight: bfloat16 [2048, 1024], P(None, 'tp'), may hold values from -6 to 6
- value_weight: bfloat16 [2048, 1024], P(None, 'tp'), may hold values from -0.125 to 0.125
- out_weight: bfloat16 [1024, 2048], P('tp'), may hold values from -0.1875 to 0.1875
- post_gain: float32 [2048], replicated, may hold values from 0.1 to 1.9
- expert_input: bfloat16 [4096, 2048], P(('grp', 'ep', 'tp')), parts along dimension 0, may hold values from -6 to 6
- expert_gain: float32 [2048], replicated, may hold values from 0.1 to 1.9
- routes: int32 [4096, 2], P(('grp', 'ep', 'tp')), parts along dimension 0, may hold values from 0 to 3, all different within a row; in each aligned block of 128 rows (0 to 127, 128 to 255, ...) at most 72 rows name the same one
- route_weight: float32 [4096, 2], P(('grp', 'ep', 'tp')), parts along dimension 0, may hold values from 0.2 to 1
- expert_gate: bfloat16 [4, 2048, 2048], P('ep', None, 'tp'), may hold values from -0.125 to 0.125
- expert_upward: bfloat16 [4, 2048, 2048], P('ep', None, 'tp'), may hold values from -0.125 to 0.125
- expert_down: bfloat16 [4, 2048, 2048], P('ep', 'tp'), may hold values from -0.125 to 0.125
Outputs:
- mixer_output: bfloat16 [4096, 2048], P(('grp', 'ep', 'tp')), parts along dimension 0
- expert_output: bfloat16 [4096, 2048], P(('grp', 'ep', 'tp')), parts along dimension 0
The draws below stay inside these ranges and needn't reach their ends.
There are 2 independent parts, one for each index of `grp`. The reference program is written for one: setup_inputs(seed, part) draws one part's arguments, and reference() takes and returns one part's arrays. A program takes and returns all parts, laid end to end along the dimension named above; an argument that names none is the same for every part. Nothing has to cross between parts.
Inputs may be any that keep to these rules, and one draw needn't show every extreme that they name: `forget_cumsum`: each head's row never rises along positions. `routes`: A row names 2 different experts. Within the rows of one device (aligned blocks of 128 rows) no expert is named by more than 72 rows, and in every draw some expert is named by exactly 72 rows of some block.
All inputs are finite; a program needn't handle non-finite values.
Results may differ from the reference program's by a relative error of at most 0.012.
Values may be sent and summed in bfloat16 or wider, within the bound.
A program may use at most 128 MiB of HBM per device.

```python
import math
import jax
import jax.numpy as jnp
import numpy as np
from jax import lax

D = 2048
ATTENDER_NUMBER = 8
HEAD_DIM = 128
EXP_FF = 2048
TOP = 2
MOE_ROWS = 128
SPAN = 512
WINDOW_EXTENT = 2048
TOK_MOE = 2048
EXPERTS = 4
CAP = 72
N_EP = 4
N_TP = 4


def draw_mixer_input(key, part):
    base = jnp.clip(jax.random.normal(jax.random.fold_in(key, 1), (WINDOW_EXTENT, D), jnp.float32), -6.0, 6.0)
    return base.astype(jnp.bfloat16)


def base_weight(key, number):
    normal = jax.random.normal(jax.random.fold_in(key, number), (D, ATTENDER_NUMBER * HEAD_DIM), jnp.float32)
    return jnp.clip(normal, -6.0, 6.0) * D ** (-0.5)


def draw_query_weight(key, part):
    return base_weight(key, 101).astype(jnp.bfloat16)


def draw_key_weight(key, part):
    return base_weight(key, 202).astype(jnp.bfloat16)


def draw_forget_cumsum(key, part):
    order = jax.random.permutation(jax.random.fold_in(key, 1), ATTENDER_NUMBER)
    fast_count = ATTENDER_NUMBER // 2
    rapid_route = order < fast_count
    fast_rate = jnp.exp(jax.random.uniform(jax.random.fold_in(key, 2), (ATTENDER_NUMBER,), jnp.float32, math.log(1.0 / 100.0), math.log(1.0 / 30.0)))
    slow_rate = 0.4 / WINDOW_EXTENT * jnp.exp(jax.random.uniform(jax.random.fold_in(key, 3), (ATTENDER_NUMBER,), jnp.float32, math.log(0.7), math.log(1.4)))
    rate = jnp.where(rapid_route, fast_rate, slow_rate)
    factor = jnp.exp(jax.random.uniform(jax.random.fold_in(key, 4), (ATTENDER_NUMBER, WINDOW_EXTENT // SPAN), jnp.float32, math.log(0.5), math.log(2.0)))
    factor = jnp.repeat(factor, SPAN, axis=1)
    jitter = jax.random.uniform(jax.random.fold_in(key, 5), (ATTENDER_NUMBER, WINDOW_EXTENT), jnp.float32, 0.3, 1.7)
    advance_increment = -rate[:, None] * factor * jitter
    flurry_slot = jax.random.randint(jax.random.fold_in(key, 6), (ATTENDER_NUMBER, 3), 0, WINDOW_EXTENT)
    flurry_extent = jnp.log(jax.random.uniform(jax.random.fold_in(key, 7), (ATTENDER_NUMBER, 3), jnp.float32, 0.5, 0.8))
    element_place = jnp.arange(WINDOW_EXTENT, dtype=jnp.int32)
    agreeing_tally = element_place[None, None, :] == flurry_slot[:, :, None]
    flurry_clusters = jnp.sum(jnp.where(agreeing_tally, flurry_extent[:, :, None], 0.0), axis=1)
    flurry_clusters = flurry_clusters * jnp.where(rapid_route, 0.0, 1.0)[:, None]
    return jnp.cumsum(advance_increment + flurry_clusters, axis=1)


def steps_of(key, dims, split, low, high):
    level = 1.0
    for dim, blocks in split:
        steps = jax.random.uniform(jax.random.fold_in(jax.random.fold_in(key, 6), dim), (blocks,), jnp.float32, low / len(split), high / len(split))
        level = level * jnp.repeat(jnp.exp(steps), dims[dim] // blocks).reshape((-1,) + (1,) * (len(dims) - 1 - dim))
    return level


def shared_out(key, own, number, rows, count, top, reach, skew):
    order = jax.random.permutation(key, count)
    packed, common = load_shares(count, rows * top, reach, skew, True), load_shares(count, rows * top, reach, skew, False)
    places = jnp.arange(count)

    def named(tallies, turn):
        used = int((tallies > 0).sum())
        fixed = max(1, used // 4)
        shifted = fixed + (places - fixed + turn * (used - fixed)) % max(1, count - fixed)
        return jnp.zeros((count,), jnp.int32).at[order[jnp.where(places < fixed, places, shifted)]].set(jnp.asarray(tallies, jnp.int32))

    tallies = jnp.where(number % 4 == 0, named(packed, number // 4), named(common, number - number // 4 - 1))
    mixed = jax.random.permutation(jax.random.fold_in(own, 3), count)
    donor, receiver = mixed[0:count // 2 * 2:2], mixed[1:count // 2 * 2:2]
    margin = jnp.minimum(tallies[donor] - 1, reach - tallies[receiver]) // 2
    margin = jnp.where((donor == order[0]) | (receiver == order[0]) | (tallies[receiver] == 0), 0, jnp.maximum(margin, 0))
    shifted = jax.random.randint(jax.random.fold_in(own, 4), (count // 2,), 0, 1 << 20) % (margin + 1)
    tallies = tallies.at[donor].add(-shifted).at[receiver].add(shifted)
    items = jnp.searchsorted(jnp.cumsum(tallies), jnp.arange(rows * top), side="right").astype(jnp.int32)
    listing = items.reshape(top, rows).T
    listing = listing[jax.random.permutation(jax.random.fold_in(own, 1), rows)]
    turn = jax.random.randint(jax.random.fold_in(own, 2), (rows, 1), 0, top)
    return jnp.take_along_axis(listing, (jnp.arange(top)[None, :] + turn) % top, axis=1)


def load_shares(amount, total, bound, skew, full):
    weights = [(1 << 20) // math.isqrt(standing ** skew) + 1 for standing in range(1, amount + 1)]
    largest = bound if full else min(bound, max(-(-total // amount), total * weights[0] // sum(weights)))
    least = 1 if total - largest >= amount - 1 else 0
    counts, surplus = [largest] + [least] * (amount - 1), total - largest - least * (amount - 1)
    while surplus > 0:
        movable = [i for i in range(1, amount) if counts[i] < largest] or [i for i in range(1, amount) if counts[i] < bound]
        mass, budget = sum([weights[i] for i in movable]), surplus
        for i in movable:
            addition = min(bound - counts[i], max(1, budget * weights[i] // mass), surplus)
            counts[i] = counts[i] + addition
            surplus = surplus - addition
    return np.array(counts)


def gaussian(stream_key, shape, scale, most, split=(), held_as=jnp.bfloat16):
    level = steps_of(stream_key, shape, split, -0.22, 0.18) if split else 1.0
    result = jax.random.normal(stream_key, shape, jnp.float32) * scale * level
    return jnp.minimum(jnp.maximum(result, -most), most).astype(held_as)


def setup_inputs(seed: int = 0, part: int = 0) -> dict:
    keys = jax.random.split(jax.random.key(seed), 16)
    own_keys = jax.random.split(jax.random.fold_in(keys[15], part), 16)
    mixer_input = draw_mixer_input(jax.random.fold_in(jax.random.fold_in(keys[15], part), 71), part)
    forget_cumsum = draw_forget_cumsum(jax.random.fold_in(jax.random.fold_in(keys[15], part), 71), part)
    mixer_gain = jnp.clip(1.0 + 0.18 * jax.random.normal(keys[2], (D,), jnp.float32), 0.1, 1.9)
    query_weight = draw_query_weight(jax.random.fold_in(keys[15], 71), part)
    key_weight = draw_key_weight(jax.random.fold_in(keys[15], 71), part)
    value_weight = gaussian(keys[5], (D, ATTENDER_NUMBER * HEAD_DIM), D ** -0.5, 0.125, ((1, 4),))
    out_weight = gaussian(keys[6], (ATTENDER_NUMBER * HEAD_DIM, D), (ATTENDER_NUMBER * HEAD_DIM) ** -0.5, 0.1875, ((0, 4),))
    post_gain = jnp.clip(1.0 + 0.18 * jax.random.normal(keys[7], (D,), jnp.float32), 0.1, 1.9)
    expert_input = gaussian(own_keys[8], (TOK_MOE, D), 1.0, 6.0, ((0, 16),))
    expert_gain = jnp.clip(1.0 + 0.18 * jax.random.normal(keys[9], (D,), jnp.float32), 0.1, 1.9)
    routes_keys = jax.random.split(jax.random.fold_in(own_keys[10], 1), TOK_MOE // MOE_ROWS)
    routes_turns = jax.random.permutation(jax.random.fold_in(own_keys[10], 3), TOK_MOE // MOE_ROWS)
    routes = jax.vmap(lambda own, number: shared_out(jax.random.fold_in(own_keys[10], 2), own, number, MOE_ROWS, EXPERTS, TOP, CAP, 2))(routes_keys, routes_turns).reshape((TOK_MOE, TOP))
    route_weight = jnp.clip(0.2 + 0.8 * jax.random.uniform(own_keys[11], (TOK_MOE, TOP), jnp.float32) ** steps_of(own_keys[11], (TOK_MOE, TOP), ((0, 16),), -0.2, 0.2), 0.2, 1.0)
    expert_gate = gaussian(keys[12], (EXPERTS, D, EXP_FF), D ** -0.5, 0.125, ((0, 4), (2, 4)))
    expert_upward = gaussian(keys[13], (EXPERTS, D, EXP_FF), D ** -0.5, 0.125, ((0, 4), (2, 4)))
    expert_down = gaussian(keys[14], (EXPERTS, EXP_FF, D), EXP_FF ** -0.5, 0.125, ((0, 4), (1, 4)))
    return dict(mixer_input=mixer_input, forget_cumsum=forget_cumsum, mixer_gain=mixer_gain, query_weight=query_weight, key_weight=key_weight, value_weight=value_weight, out_weight=out_weight, post_gain=post_gain, expert_input=expert_input, expert_gain=expert_gain, routes=routes, route_weight=route_weight, expert_gate=expert_gate, expert_upward=expert_upward, expert_down=expert_down)


EPS = 1e-06
MASKED = -1e+30

def normalize(rows, gain):
    values = rows.astype(jnp.float32)
    inverse = lax.rsqrt(lax.optimization_barrier(jnp.mean(values * values, axis=-1, keepdims=True)) + EPS)
    return values * inverse * gain.astype(jnp.float32)

def attend(queries, key_rows, value_rows, forget_cumsum):
    head_q = queries.reshape(WINDOW_EXTENT, ATTENDER_NUMBER, HEAD_DIM).transpose(1, 0, 2).astype(jnp.float32)
    head_k = key_rows.reshape(WINDOW_EXTENT, ATTENDER_NUMBER, HEAD_DIM).transpose(1, 0, 2).astype(jnp.float32)
    head_v = value_rows.reshape(WINDOW_EXTENT, ATTENDER_NUMBER, HEAD_DIM).transpose(1, 0, 2).astype(jnp.float32)
    block_size = math.gcd(WINDOW_EXTENT, 512)

    def one_query_block(block_index):
        first_row = block_index * block_size
        query_block = lax.dynamic_slice_in_dim(head_q, first_row, block_size, 1)
        query_gate = lax.dynamic_slice_in_dim(forget_cumsum, first_row, block_size, 1)
        query_pos = first_row + jnp.arange(block_size, dtype=jnp.int32)

        def advance_increment(key_index, state):
            running_max, running_sum, running_acc = state
            key_first = key_index * block_size
            key_block = lax.dynamic_slice_in_dim(head_k, key_first, block_size, 1)
            value_block = lax.dynamic_slice_in_dim(head_v, key_first, block_size, 1)
            key_gate = lax.dynamic_slice_in_dim(forget_cumsum, key_first, block_size, 1)
            scores = jnp.einsum('hqd,hkd->hqk', query_block, key_block) * HEAD_DIM ** (-0.5)
            scores = scores + query_gate[:, :, None] - key_gate[:, None, :]
            key_pos = key_first + jnp.arange(block_size, dtype=jnp.int32)
            visible = (key_pos[None, :] <= query_pos[:, None])[None]
            scores = jnp.where(visible, scores, MASKED)
            new_max = jnp.maximum(running_max, lax.optimization_barrier(jnp.max(scores, axis=-1)))
            weights = jnp.where(visible, jnp.exp(scores - new_max[..., None]), 0.0)
            rescale = jnp.exp(running_max - new_max)
            running_sum = running_sum * rescale + lax.optimization_barrier(jnp.sum(weights, axis=-1))
            rounded = lax.optimization_barrier(weights.astype(jnp.bfloat16)).astype(jnp.float32)
            running_acc = running_acc * rescale[..., None] + jnp.einsum('hqk,hkd->hqd', rounded, value_block)
            return (new_max, running_sum, running_acc)
        initial = (jnp.full((ATTENDER_NUMBER, block_size), MASKED, jnp.float32), jnp.zeros((ATTENDER_NUMBER, block_size), jnp.float32), jnp.zeros((ATTENDER_NUMBER, block_size, HEAD_DIM), jnp.float32))
        running_max, running_sum, running_acc = lax.fori_loop(0, block_index + 1, advance_increment, initial)
        return (running_acc / running_sum[..., None]).astype(jnp.bfloat16)
    blocks = lax.map(one_query_block, jnp.arange(WINDOW_EXTENT // block_size, dtype=jnp.int32))
    return blocks.transpose(0, 2, 1, 3).reshape(WINDOW_EXTENT, ATTENDER_NUMBER * HEAD_DIM)

def one_expert(operands):
    rows, gate_part, upward_part, down_part = operands
    group = EXP_FF // N_TP
    running = jnp.zeros((rows.shape[0], D), jnp.float32)
    for shard in range(N_TP):
        gate_proj = jnp.dot(rows, gate_part[:, shard * group:(shard + 1) * group], preferred_element_type=jnp.float32)
        upward = jnp.dot(rows, upward_part[:, shard * group:(shard + 1) * group], preferred_element_type=jnp.float32)
        hidden = (jax.nn.silu(gate_proj) * upward).astype(jnp.bfloat16)
        partial_term = jnp.dot(hidden, down_part[shard * group:(shard + 1) * group, :], preferred_element_type=jnp.float32)
        running = running + lax.optimization_barrier(partial_term.astype(jnp.bfloat16)).astype(jnp.float32)
    return running.astype(jnp.bfloat16)

def reference(mixer_input, forget_cumsum, mixer_gain, query_weight, key_weight, value_weight, out_weight, post_gain, expert_input, expert_gain, routes, route_weight, expert_gate, expert_upward, expert_down):
    normed = normalize(mixer_input, mixer_gain).astype(jnp.bfloat16)
    queries = jnp.dot(normed, query_weight, preferred_element_type=jnp.float32).astype(jnp.bfloat16)
    key_rows = jnp.dot(normed, key_weight, preferred_element_type=jnp.float32).astype(jnp.bfloat16)
    value_rows = jnp.dot(normed, value_weight, preferred_element_type=jnp.float32).astype(jnp.bfloat16)
    attended = attend(queries, key_rows, value_rows, forget_cumsum)
    group = ATTENDER_NUMBER * HEAD_DIM // N_TP
    mixer_sum = jnp.zeros((WINDOW_EXTENT, D), jnp.float32)
    for shard in range(N_TP):
        partial_term = jnp.dot(attended[:, shard * group:(shard + 1) * group], out_weight[shard * group:(shard + 1) * group, :], preferred_element_type=jnp.float32)
        mixer_sum = mixer_sum + lax.optimization_barrier(partial_term.astype(jnp.bfloat16)).astype(jnp.float32)
    mixer_output = normalize(mixer_sum, post_gain).astype(jnp.bfloat16)
    sources = N_EP * N_TP
    normed_moe = normalize(expert_input, expert_gain).astype(jnp.bfloat16)
    grouped = routes.reshape(sources, MOE_ROWS * TOP).astype(jnp.int32)
    member = (grouped[:, :, None] == jnp.arange(EXPERTS, dtype=jnp.int32)[None, None, :]).astype(jnp.int32)
    before = jnp.cumsum(member, axis=1) - member
    slot_rank = lax.optimization_barrier(jnp.sum(before * member, axis=-1))
    slot_index = grouped * (sources * CAP) + jnp.arange(sources, dtype=jnp.int32)[:, None] * CAP + slot_rank
    slot_index = slot_index.reshape(-1).astype(jnp.int32)
    repeated = jnp.repeat(normed_moe, TOP, axis=0)
    buffer = jnp.zeros((EXPERTS * sources * CAP, D), jnp.bfloat16).at[slot_index].set(repeated)
    buffer = buffer.reshape(EXPERTS, sources * CAP, D)
    outputs = lax.map(one_expert, (buffer, expert_gate, expert_upward, expert_down)).reshape(-1, D)
    picked = outputs[slot_index].reshape(TOK_MOE, TOP, D).astype(jnp.float32)
    expert_output = lax.optimization_barrier(jnp.sum(picked * route_weight.astype(jnp.float32)[:, :, None], axis=1)).astype(jnp.bfloat16)
    return (mixer_output, expert_output)
```

```python
import functools

import jax
import jax.numpy as jnp
from jax import lax
from jax.experimental import pallas as pl
from jax.experimental.pallas import tpu as pltpu
from jax.sharding import PartitionSpec as P

EPS = 1e-06
MASKED = -1e30
MESH = pl.DeviceIdType.MESH
F32 = jnp.float32
BF16 = jnp.bfloat16
ROW_TILE = 8
LANES = 128
LOG2_E = 1.4426950408889634


def normalize(row_block, gain):
    values = row_block.astype(F32)
    inverse = lax.rsqrt(jnp.mean(values * values, axis=-1, keepdims=True) + EPS)
    return values * inverse * gain


def iota(shape, dim):
    return lax.broadcasted_iota(jnp.int32, shape, dim)


def columns_of(rows):
    spread = jnp.broadcast_to(rows[0:1], (LANES, rows.shape[1]))
    which = iota(spread.shape, 0)
    for h in range(1, rows.shape[0]):
        spread = jnp.where(which == h, rows[h : h + 1], spread)
    return spread.T


def kernel(
    n_ep,
    head_dim,
    refs,
):
    r = refs
    me = lax.axis_index("ep")
    t = lax.axis_index("tp")
    hi = t // 2
    lo = t % 2
    lo_peer = 2 * hi + (1 - lo)
    hi_peer = 2 * (1 - hi) + lo
    other_hi = 1 - hi
    seg, queries, kv, rows, out = r["seg"], r["queries"], r["kv"], r["rows"], r["out"]
    hid, res, drec, erec, fin, ret = r["hid"], r["res"], r["drec"], r["erec"], out, r["ret"]
    run_max, run_sum, run_acc, attended = r["run_max"], r["run_sum"], r["run_acc"], r["attended"]
    mdrec, merec, gate, columns = r["mdrec"], r["mixer_input"], r["gate"], r["columns"]
    wq, wk, wv, wo, eg, eu, ed = (r[k] for k in ("wq", "wk", "wv", "wo", "eg", "eu", "ed"))
    mix_rows, width = r["mixer_out"].shape
    head_width = wq.shape[1]
    heads = head_width // head_dim
    span = 4 * mix_rows
    cap = out.shape[1]
    top_count, moe_rows = r["routes"].shape
    folded = n_ep == 4

    def remote(src, dst, send_sem, recv_sem, where):
        return pltpu.make_async_remote_copy(
            src_ref=src,
            dst_ref=dst,
            send_sem=send_sem,
            recv_sem=recv_sem,
            device_id=where,
            device_id_type=MESH,
        )

    names = (
        "mixer_input", "mixer_gain", "routes", "expert_input", "expert_gain", "wq", "wk", "wv",
        "eg", "eu", "ed", "route_weight", "gate", "post_gain", "wo",
    )
    loads = {
        name: pltpu.make_async_copy(r[name + "_hbm"], r[name], r["load_sem"].at[i])
        for i, name in enumerate(names)
    }
    barrier = pltpu.get_barrier_semaphore()
    pl.semaphore_signal(barrier, inc=1, device_id={"tp": lo_peer}, device_id_type=MESH)
    pl.semaphore_signal(barrier, inc=1, device_id={"tp": hi_peer}, device_id_type=MESH)

    @pl.loop(1, n_ep)
    def _(j):
        pl.semaphore_signal(barrier, inc=1, device_id={"ep": lax.rem(me + j, n_ep)}, device_id_type=MESH)

    for name in names:
        loads[name].start()

    n_hi = remote(seg.at[t], seg.at[t], r["ns"].at[0], r["nr"].at[0], {"tp": hi_peer})
    n_lo = remote(seg.at[t], seg.at[t], r["ns"].at[1], r["nr"].at[1], {"tp": lo_peer})
    n_relay = remote(seg.at[hi_peer], seg.at[hi_peer], r["ns"].at[2], r["nr"].at[2], {"tp": lo_peer})
    diag_peer = 2 * other_hi + (1 - lo)

    def copy_a(to):
        return remote(out.at[to], rows.at[me, t], r["as"].at[to], r["ar"].at[me], {"ep": to})

    def recv_a(s):
        return remote(out.at[s], rows.at[s, t], r["as"].at[s], r["ar"].at[s], {"ep": s})

    def copy_b_hi(s):
        return remote(rows.at[s, t], rows.at[s, t], r["bs"].at[0, s], r["br"].at[0, s], {"tp": hi_peer})

    def copy_b_lo(s):
        return remote(rows.at[s, t], rows.at[s, t], r["bs"].at[1, s], r["br"].at[1, s], {"tp": lo_peer})

    def copy_c(s):
        return remote(rows.at[s, hi_peer], rows.at[s, hi_peer], r["cs"].at[s], r["cr"].at[s], {"tp": lo_peer})

    def copy_d(s, h):
        return remote(res.at[s, 2 * h + (1 - lo)], drec.at[s, h], r["ds"].at[h, s], r["dr"].at[h, s], {"tp": lo_peer})

    def copy_e(s):
        return remote(drec.at[s, other_hi], erec.at[s], r["es"].at[s], r["er"].at[s], {"tp": hi_peer})

    def copy_f(s):
        return remote(fin.at[s], ret.at[me], r["fs"].at[s], r["fr"].at[me], {"ep": s})

    def recv_f(e):
        return remote(fin.at[e], ret.at[e], r["fs"].at[e], r["fr"].at[e], {"ep": e})

    def copy_kv(b, to):
        return remote(kv.at[b], kv.at[b], r["ks"].at[b], r["kr"].at[b], {"ep": to})

    loads["mixer_input"].wait()
    loads["mixer_gain"].wait()
    seg[t] = normalize(r["mixer_input"][...], r["mixer_gain"][...]).astype(BF16)
    pl.semaphore_wait(barrier, 2 + n_ep - 1)
    n_hi.start()
    n_lo.start()

    loads["routes"].wait()
    loads["expert_input"].wait()
    loads["expert_gain"].wait()
    experts = (n_ep + 15) // 16 * 16
    expert_ids = iota((experts, moe_rows), 0)
    chosen = [expert_ids == r["routes"][k : k + 1, :] for k in range(top_count)]
    member = functools.reduce(jnp.logical_or, chosen)
    earlier = jnp.where(iota((moe_rows, moe_rows), 0) < iota((moe_rows, moe_rows), 1), 1.0, 0.0)
    rank = jnp.dot(
        jnp.where(member, 1.0, 0.0).astype(BF16), earlier.astype(BF16), preferred_element_type=F32
    )
    slot = jnp.where(member, rank, -1.0)
    slot_rows = iota((cap, moe_rows), 0).astype(F32)
    for e in range(n_ep):
        r["dispatch"][e] = jnp.where(slot[e : e + 1, :] == slot_rows, 1.0, 0.0).astype(BF16)
    normed_moe = r["expert_input"]
    normed_moe[...] = normalize(normed_moe[...], r["expert_gain"][...]).astype(BF16)

    sent = r["dispatch"][...].reshape(n_ep * cap, moe_rows)
    out[...] = jnp.dot(sent, normed_moe[...], preferred_element_type=F32).astype(BF16).reshape(out.shape)
    if folded:
        s1 = me + 1 - 2 * (me % 2)
        s2 = jnp.where(me < 2, 3, 0)
        s3 = jnp.where(me < 2, 2, 1)
        for s in (s1, s2, s3):
            copy_a(s).start()
    else:

        @pl.loop(1, n_ep)
        def _(j):
            copy_a(lax.rem(me + j, n_ep)).start()

    rows[me, t] = out[me]
    copy_b_hi(me).start()
    copy_b_lo(me).start()

    loads["route_weight"].wait()
    weight = functools.reduce(
        lambda a, b: a + b,
        [jnp.where(chosen[k], r["route_weight"][k : k + 1, :], 0.0) for k in range(top_count)],
    )

    def turned(x):
        return jnp.concatenate([x, jnp.zeros((LANES - experts, moe_rows), F32)], axis=0).T

    slot_turned = turned(slot)
    r["weights"][...] = turned(weight)
    slot_columns = iota((moe_rows, cap), 1).astype(F32)
    for e in range(n_ep):
        r["pick"][e] = jnp.where(slot_turned[:, e : e + 1] == slot_columns, 1.0, 0.0).astype(BF16)

    def combine(e, first):
        weights = r["weights"][...]
        share = jnp.sum(jnp.where(iota(weights.shape, 1) == e, weights, 0.0), axis=1, keepdims=True)

        y = share * jnp.dot(r["pick"][e], ret[e], preferred_element_type=F32)
        r["combined"][...] = y if first else r["combined"][...] + y

    def project_in(half):
        x = seg[pl.ds(2 * half, 2)].reshape(2 * mix_rows, width)
        p = pl.ds(pl.multiple_of(half * 2 * mix_rows, 2 * mix_rows), 2 * mix_rows)
        kv[me, p, pl.ds(0, head_width)] = jnp.dot(x, wk[...], preferred_element_type=F32).astype(BF16)
        kv[me, p, pl.ds(head_width, head_width)] = jnp.dot(x, wv[...], preferred_element_type=F32).astype(BF16)
        queries[p, :] = jnp.dot(x, wq[...], preferred_element_type=F32).astype(BF16)

    def expert(s, half):
        x = rows[s, pl.ds(2 * half, 2)].reshape(2 * cap, width)
        g = jnp.dot(x, eg[...], preferred_element_type=F32)
        u = jnp.dot(x, eu[...], preferred_element_type=F32)
        hid[...] = (g / (1.0 + jnp.exp(-g)) * u).astype(BF16)
        y = jnp.dot(hid[...], ed[...], preferred_element_type=F32)
        res[s, pl.ds(2 * half, 2)] = y.astype(BF16).reshape(2, cap, width)
        copy_d(s, half).start()

    def step_e(s):
        copy_d(s, other_hi).wait_recv()
        drec[s, other_hi] = (res[s, hi_peer].astype(F32) + drec[s, other_hi].astype(F32)).astype(BF16)
        copy_e(s).start()

    def step_f(s, own):
        copy_d(s, hi).wait_recv()
        copy_e(s).wait_recv()
        total = (res[s, t].astype(F32) + drec[s, hi].astype(F32) + erec[s].astype(F32)).astype(BF16)
        if own:
            ret[s] = total
        else:
            copy_a(s).wait_send()
            fin[s] = total
            copy_f(s).start()

    scale = head_dim ** (-0.5) * LOG2_E

    def block(b):
        return pl.ds(pl.multiple_of(b * span, span), span)

    def attend(q, qb, b, cols, i, masked, first):
        for h in range(heads):
            hc = pl.ds(h * head_dim, head_dim)
            vc = pl.ds(head_width + h * head_dim, head_dim)
            s = lax.dot_general(kv[b, :, hc], q[:, hc], (((1,), (1,)), ((), ())), preferred_element_type=F32)
            s = s * scale + (gate[h : h + 1, block(qb)] - cols[:, h : h + 1])
            if masked:
                s = jnp.where(iota(s.shape, 0) <= iota(s.shape, 1), s, MASKED)
            new = jnp.max(s, axis=0, keepdims=True)
            if not first:
                old = run_max[i, h : h + 1]
                new = jnp.maximum(old, new)
                fix = jnp.exp2(old - new)
            w = jnp.exp2(s - new)
            part_sum = jnp.sum(w, axis=0, keepdims=True)
            part_acc = lax.dot_general(
                kv[b, :, vc], w.astype(BF16), (((0,), (0,)), ((), ())), preferred_element_type=F32
            )
            run_max[i, h : h + 1] = new
            if first:
                run_sum[i, h : h + 1] = part_sum
                run_acc[i, h] = part_acc
            else:
                run_sum[i, h : h + 1] = run_sum[i, h : h + 1] * fix + part_sum
                run_acc[i, h] = run_acc[i, h] * fix + part_acc

    def finish():
        for h in range(heads):
            mean = run_acc[0, h] / run_sum[0, h : h + 1]
            attended[:, pl.ds(h * head_dim, head_dim)] = mean.T.astype(BF16)

    def load_gate():
        loads["gate"].wait()
        gate[...] = gate[...] * LOG2_E

    def gate_columns(i, b):
        columns[i] = columns_of(gate[:, block(b)])

    part = seg

    def project(b):
        x = attended[pl.ds(pl.multiple_of(b * mix_rows, mix_rows), mix_rows), :]

        part[b] = jnp.dot(x, wo[...], preferred_element_type=F32).astype(BF16)

    def copy_m(h):
        return remote(part.at[2 * h + (1 - lo)], mdrec.at[h], r["ms"].at[h], r["mr"].at[h], {"tp": lo_peer})

    m_hi = remote(mdrec.at[other_hi], merec, r["ms"].at[2], r["mr"].at[2], {"tp": hi_peer})

    def mix_out():
        loads["wo"].wait()
        n_hi.wait_send()
        n_lo.wait_send()
        n_relay.wait_send()
        project(diag_peer)
        copy_m(other_hi).start()
        project(hi_peer)
        copy_m(other_hi).wait_recv()
        mdrec[other_hi] = (part[hi_peer].astype(F32) + mdrec[other_hi].astype(F32)).astype(BF16)
        m_hi.start()
        project(lo_peer)
        copy_m(hi).start()
        project(t)

    def mix_end():
        copy_m(hi).wait_recv()
        loads["post_gain"].wait()
        m_hi.wait_recv()
        total = part[t].astype(F32) + mdrec[hi].astype(F32) + merec[...].astype(F32)
        inverse = lax.rsqrt(jnp.mean(total * total, axis=-1, keepdims=True) + EPS)
        r["mixer_out"][...] = (total * inverse * r["post_gain"][...]).astype(BF16)

    def relay_b(s):
        recv_a(s).wait_recv()
        copy_b_hi(s).start()
        copy_b_lo(s).start()

    def relay_c(s):
        copy_b_hi(s).wait_recv()
        copy_c(s).start()

    def expert_own(s):
        copy_b_lo(s).wait_recv()
        expert(s, hi)

    def expert_other(s):
        copy_c(s).wait_recv()
        expert(s, other_hi)

    if folded:
        qin, obuf, lbuf, oin, lin = r["qin"], r["obuf"], r["lbuf"], r["oin"], r["lin"]
        helper = me == 1
        odd = me % 2 == 1
        asks = me >= 2

        def copy_q():
            return remote(queries, qin.at[me - 2], r["qs"].at[0], r["qr"].at[me - 2], {"ep": 1})

        def recv_q(i):
            return remote(queries, qin.at[i], r["qs"].at[0], r["qr"].at[i], {"ep": 1})

        def copy_o(i):
            return remote(obuf.at[i], oin, r["os"].at[0, i], r["or"].at[0], {"ep": 2 + i})

        def copy_l(i):
            return remote(lbuf.at[i], lin, r["os"].at[1, i], r["or"].at[1], {"ep": 2 + i})

        for name in ("wq", "wk", "wv"):
            loads[name].wait()
        n_lo.wait_recv()
        project_in(hi)
        for name in ("eg", "eu", "ed"):
            loads[name].wait()
        expert_own(me)
        load_gate()
        gate_columns(0, me)

        @pl.when(odd)
        def _():
            gate_columns(1, me - 1)

        relay_b(s1)
        n_hi.wait_recv()
        n_relay.start()
        expert_own(s1)
        n_relay.wait_recv()
        project_in(other_hi)

        @pl.when(asks)
        def _():
            copy_q().start()

        @pl.when(me % 2 == 0)
        def _():
            copy_kv(me, me + 1).start()

        relay_c(me)
        attend(queries, me, me, columns.at[0], 0, True, True)
        relay_b(s2)
        expert_other(me)
        expert_own(s2)
        relay_c(s1)
        expert_other(s1)
        step_e(s1)

        @pl.when(helper)
        def _():
            for i in range(2):
                recv_q(i).wait_recv()
                attend(qin.at[i], 2 + i, me, columns.at[0], 1 + i, False, True)

        relay_c(s2)
        expert_other(s2)
        step_e(s2)
        relay_b(s3)

        @pl.when(odd)
        def _():
            copy_kv(me - 1, me).wait_recv()

        @pl.when(helper)
        def _():
            for i in range(2):
                attend(qin.at[i], 2 + i, 0, columns.at[1], 1 + i, False, False)
                for h in range(heads):
                    total = run_sum[1 + i, h : h + 1]
                    obuf[i, pl.ds(h * head_dim, head_dim)] = (run_acc[1 + i, h] / total).astype(BF16)
                    lbuf[i, h : h + 1] = run_max[1 + i, h : h + 1] + jnp.log2(total)
                copy_o(i).start()
                copy_l(i).start()

        @pl.when(odd)
        def _():
            attend(queries, me, me - 1, columns.at[1], 0, False, False)

        expert_own(s3)

        @pl.when(me < 2)
        def _():
            finish()

        step_f(s1, False)
        relay_c(s3)
        expert_other(s3)
        step_e(s3)
        step_e(me)
        step_f(s2, False)

        @pl.when(asks)
        def _():
            copy_o(me - 2).wait_recv()
            copy_l(me - 2).wait_recv()
            for h in range(heads):
                hc = pl.ds(h * head_dim, head_dim)
                far, old = lin[h : h + 1], run_max[0, h : h + 1]
                new = jnp.maximum(old, far)
                fix, far_fix = jnp.exp2(old - new), jnp.exp2(far - new)
                numer = run_acc[0, h] * fix + oin[hc].astype(F32) * far_fix
                attended[:, hc] = (numer / (run_sum[0, h : h + 1] * fix + far_fix)).T.astype(BF16)

        mix_out()
        step_f(s3, False)
        step_f(me, True)
        combine(me, True)
        for e in (s1, s2, s3):
            recv_f(e).wait_recv()
            combine(e, False)
        r["expert_out"][...] = r["combined"][...].astype(BF16)
        mix_end()

        @pl.when(asks)
        def _():
            copy_q().wait_send()

        @pl.when(me % 2 == 0)
        def _():
            copy_kv(me, me + 1).wait_send()

        @pl.when(helper)
        def _():
            for i in range(2):
                copy_o(i).wait_send()
                copy_l(i).wait_send()

    else:
        step = lambda j: lax.rem(me + j, n_ep)
        for name in ("wq", "wk", "wv"):
            loads[name].wait()
        n_hi.wait_recv()
        n_relay.start()
        n_lo.wait_recv()
        project_in(hi)
        n_relay.wait_recv()
        project_in(other_hi)

        @pl.when(me + 1 < n_ep)
        def _():
            copy_kv(me, me + 1).start()

        for name in ("eg", "eu", "ed"):
            loads[name].wait()
        load_gate()
        gate_columns(0, me)

        @pl.loop(0, n_ep)
        def _(j):
            s = step(j)

            @pl.when(j + 1 < n_ep)
            def _():
                relay_b(step(j + 1))

            expert_own(s)
            relay_c(s)
            expert_other(s)

            @pl.when(j >= 1)
            def _():
                step_e(step(j - 1))

            @pl.when((j >= 1) & (j < n_ep - 1) & (me - j >= 0))
            def _():
                copy_kv(me - j, me).wait_recv()

                @pl.when(me + 1 < n_ep)
                def _():
                    copy_kv(me - j, me + 1).start()

        step_e(step(n_ep - 1))
        attend(queries, me, me, columns.at[0], 0, True, True)
        step_f(me, True)
        combine(me, True)

        @pl.loop(1, n_ep)
        def _(j):
            step_f(step(j), False)

        @pl.loop(1, me + 1)
        def _(d):
            @pl.when(d == n_ep - 1)
            def _():
                copy_kv(0, me).wait_recv()

            gate_columns(0, me - d)
            attend(queries, me, me - d, columns.at[0], 0, False, False)

        finish()
        mix_out()

        @pl.loop(1, n_ep)
        def _(j):
            recv_f(step(j)).wait_recv()
            combine(step(j), False)

        r["expert_out"][...] = r["combined"][...].astype(BF16)
        mix_end()

        @pl.when(me + 1 < n_ep)
        def _():
            @pl.loop(0, me + 1)
            def _(b):
                copy_kv(b, me + 1).wait_send()

    copy_m(0).wait_send()
    copy_m(1).wait_send()
    m_hi.wait_send()

    @pl.loop(0, n_ep)
    def _(j):
        s = lax.rem(me + j, n_ep)

        @pl.when(j > 0)
        def _():
            copy_f(s).wait_send()

        copy_b_hi(s).wait_send()
        copy_b_lo(s).wait_send()
        copy_c(s).wait_send()
        copy_d(s, 0).wait_send()
        copy_d(s, 1).wait_send()
        copy_e(s).wait_send()


def on_device(
    mixer_input,
    forget_cumsum,
    mixer_gain,
    query_weight,
    key_weight,
    value_weight,
    out_weight,
    post_gain,
    expert_input,
    expert_gain,
    routes,
    route_weight,
    expert_gate,
    expert_upward,
    expert_down,
):
    n_ep = lax.axis_size("ep")
    n_tp = lax.axis_size("tp")
    mix_rows, width = mixer_input.shape
    heads = forget_cumsum.shape[0]
    head_width = query_weight.shape[1]
    head_dim = head_width // heads
    span = mix_rows * n_tp
    moe_rows, top_count = routes.shape
    assert n_tp == 4 and expert_gate.shape[0] == 1
    capacity = (moe_rows * top_count * 9 + 8 * n_ep - 1) // (8 * n_ep)
    cap = (capacity + ROW_TILE - 1) // ROW_TILE * ROW_TILE
    f_width = expert_gate.shape[2]
    folded = n_ep == 4
    sets = 3 if folded else 1

    inputs = {
        "mixer_input": mixer_input,
        "mixer_gain": mixer_gain.reshape(1, -1),
        "routes": routes.T,
        "expert_input": expert_input,
        "expert_gain": expert_gain.reshape(1, -1),
        "wq": query_weight,
        "wk": key_weight,
        "wv": value_weight,
        "eg": expert_gate[0],
        "eu": expert_upward[0],
        "ed": expert_down[0],
        "route_weight": route_weight.T,
        "gate": forget_cumsum,
        "post_gain": post_gain.reshape(1, -1),
        "wo": out_weight,
    }
    vmem, dma = pltpu.VMEM, pltpu.SemaphoreType.DMA
    scratch = {name: vmem(x.shape, x.dtype) for name, x in inputs.items()}
    scratch |= {
        "seg": vmem((4, mix_rows, width), BF16),
        "queries": vmem((span, head_width), BF16),
        "kv": vmem((n_ep, span, 2 * head_width), BF16),
        "rows": vmem((n_ep, 4, cap, width), BF16),
        "out": vmem((n_ep, cap, width), BF16),
        "dispatch": vmem((n_ep, cap, moe_rows), BF16),
        "pick": vmem((n_ep, moe_rows, cap), BF16),
        "weights": vmem((moe_rows, LANES), F32),
        "combined": vmem((moe_rows, width), F32),
        "hid": vmem((2 * cap, f_width), BF16),
        "res": vmem((n_ep, 4, cap, width), BF16),
        "drec": vmem((n_ep, 2, cap, width), BF16),
        "erec": vmem((n_ep, cap, width), BF16),
        "ret": vmem((n_ep, cap, width), BF16),
        "run_max": vmem((sets, heads, span), F32),
        "run_sum": vmem((sets, heads, span), F32),
        "run_acc": vmem((sets, heads, head_dim, span), F32),
        "attended": vmem((span, head_width), BF16),
        "columns": vmem((2 if folded else 1, span, LANES), F32),
        "mdrec": vmem((2, mix_rows, width), BF16),
        "load_sem": dma((len(inputs),)),
    }
    if folded:
        scratch |= {
            "qin": vmem((2, span, head_width), BF16),
            "obuf": vmem((2, head_width, span), BF16),
            "lbuf": vmem((2, 8, span), F32),
            "oin": vmem((head_width, span), BF16),
            "lin": vmem((8, span), F32),
            "qs": dma((1,)),
            "qr": dma((2,)),
            "os": dma((2, 2)),
            "or": dma((2,)),
        }
    scratch |= {"ns": dma((3,)), "nr": dma((3,)), "ms": dma((3,)), "mr": dma((3,))}
    for name in ("a", "c", "e", "f", "k"):
        scratch |= {name + "s": dma((n_ep,)), name + "r": dma((n_ep,))}
    for name in ("b", "d"):
        scratch |= {name + "s": dma((2, n_ep)), name + "r": dma((2, n_ep))}

    labels = [name + "_hbm" for name in inputs] + ["mixer_out", "expert_out"] + list(scratch)

    def body(*refs):
        kernel(n_ep, head_dim, dict(zip(labels, refs, strict=True)))

    block = pl.BlockSpec(memory_space=pltpu.VMEM)
    return pl.pallas_call(
        body,
        out_shape=(
            jax.ShapeDtypeStruct((mix_rows, width), BF16),
            jax.ShapeDtypeStruct((moe_rows, width), BF16),
        ),
        in_specs=[pl.BlockSpec(memory_space=pl.ANY)] * len(inputs),
        out_specs=(block, block),
        scratch_shapes=list(scratch.values()),
        compiler_params=pltpu.CompilerParams(
            collective_id=0, has_side_effects=True, vmem_limit_bytes=66_500_000
        ),
    )(*inputs.values())


def solution(mesh):
    rows = P(("grp", "ep", "tp"), None)
    in_specs = (
        rows,
        P("tp", "grp"),
        P(),
        P(None, "tp"),
        P(None, "tp"),
        P(None, "tp"),
        P("tp", None),
        P(),
        rows,
        P(),
        rows,
        rows,
        P("ep", None, "tp"),
        P("ep", None, "tp"),
        P("ep", "tp", None),
    )
    return jax.shard_map(
        on_device, mesh=mesh, in_specs=in_specs, out_specs=(rows, rows), check_vma=False
    )
```

```python
import functools

import jax
import jax.numpy as jnp
from jax import lax
from jax.experimental import pallas as pl
from jax.experimental.pallas import tpu as pltpu
from jax.sharding import PartitionSpec as P

EPS = 1e-06
MASKED = -1e30
MESH = pl.DeviceIdType.MESH
F32 = jnp.float32
BF16 = jnp.bfloat16
ROW_TILE = 8
LANES = 128
LOG2_E = 1.4426950408889634


def normalize(row_block, gain):
    values = row_block.astype(F32)
    inverse = lax.rsqrt(jnp.mean(values * values, axis=-1, keepdims=True) + EPS)
    return values * inverse * gain


def iota(shape, dim):
    return lax.broadcasted_iota(jnp.int32, shape, dim)


def columns_of(rows):
    spread = jnp.broadcast_to(rows[0:1], (LANES, rows.shape[1]))
    which = iota(spread.shape, 0)
    for h in range(1, rows.shape[0]):
        spread = jnp.where(which == h, rows[h : h + 1], spread)
    return spread.T


def kernel(
    n_ep,
    head_dim,
    refs,
):
    r = refs
    me = lax.axis_index("ep")
    t = lax.axis_index("tp")
    hi = t // 2
    lo = t % 2
    lo_peer = 2 * hi + (1 - lo)
    hi_peer = 2 * (1 - hi) + lo
    other_hi = 1 - hi
    seg, queries, kv, rows, out = r["seg"], r["queries"], r["kv"], r["rows"], r["out"]
    hid, res, drec, erec, fin, ret = r["hid"], r["res"], r["drec"], r["erec"], out, r["ret"]
    run_max, run_sum, run_acc, attended = r["run_max"], r["run_sum"], r["run_acc"], r["attended"]
    mdrec, merec, gate, columns = r["mdrec"], r["mixer_input"], r["gate"], r["columns"]
    wq, wk, wv, wo, eg, eu, ed = (r[k] for k in ("wq", "wk", "wv", "wo", "eg", "eu", "ed"))
    mix_rows, width = r["mixer_out"].shape
    head_width = wq.shape[1]
    heads = head_width // head_dim
    span = 4 * mix_rows
    cap = out.shape[1]
    top_count, moe_rows = r["routes"].shape
    folded = n_ep == 4

    def remote(src, dst, send_sem, recv_sem, where):
        return pltpu.make_async_remote_copy(
            src_ref=src,
            dst_ref=dst,
            send_sem=send_sem,
            recv_sem=recv_sem,
            device_id=where,
            device_id_type=MESH,
        )

    names = (
        "mixer_input", "mixer_gain", "routes", "expert_input", "expert_gain", "wq", "wk", "wv",
        "eg", "eu", "ed", "route_weight", "gate", "post_gain", "wo",
    )
    loads = {
        name: pltpu.make_async_copy(r[name + "_hbm"], r[name], r["load_sem"].at[i])
        for i, name in enumerate(names)
    }
    barrier = pltpu.get_barrier_semaphore()
    pl.semaphore_signal(barrier, inc=1, device_id={"tp": lo_peer}, device_id_type=MESH)
    pl.semaphore_signal(barrier, inc=1, device_id={"tp": hi_peer}, device_id_type=MESH)

    @pl.loop(1, n_ep)
    def _(j):
        pl.semaphore_signal(barrier, inc=1, device_id={"ep": lax.rem(me + j, n_ep)}, device_id_type=MESH)

    for name in names:
        loads[name].start()

    n_hi = remote(seg.at[t], seg.at[t], r["ns"].at[0], r["nr"].at[0], {"tp": hi_peer})
    n_lo = remote(seg.at[t], seg.at[t], r["ns"].at[1], r["nr"].at[1], {"tp": lo_peer})
    n_relay = remote(seg.at[hi_peer], seg.at[hi_peer], r["ns"].at[2], r["nr"].at[2], {"tp": lo_peer})
    diag_peer = 2 * other_hi + (1 - lo)

    def copy_a(to):
        return remote(out.at[to], rows.at[me, t], r["as"].at[to], r["ar"].at[me], {"ep": to})

    def recv_a(s):
        return remote(out.at[s], rows.at[s, t], r["as"].at[s], r["ar"].at[s], {"ep": s})

    def copy_b_hi(s):
        return remote(rows.at[s, t], rows.at[s, t], r["bs"].at[0, s], r["br"].at[0, s], {"tp": hi_peer})

    def copy_b_lo(s):
        return remote(rows.at[s, t], rows.at[s, t], r["bs"].at[1, s], r["br"].at[1, s], {"tp": lo_peer})

    def copy_c(s):
        return remote(rows.at[s, hi_peer], rows.at[s, hi_peer], r["cs"].at[s], r["cr"].at[s], {"tp": lo_peer})

    def copy_d(s, h):
        return remote(res.at[s, 2 * h + (1 - lo)], drec.at[s, h], r["ds"].at[h, s], r["dr"].at[h, s], {"tp": lo_peer})

    def copy_e(s):
        return remote(drec.at[s, other_hi], erec.at[s], r["es"].at[s], r["er"].at[s], {"tp": hi_peer})

    def copy_f(s):
        return remote(fin.at[s], ret.at[me], r["fs"].at[s], r["fr"].at[me], {"ep": s})

    def recv_f(e):
        return remote(fin.at[e], ret.at[e], r["fs"].at[e], r["fr"].at[e], {"ep": e})

    def copy_kv(b, to):
        return remote(kv.at[b], kv.at[b], r["ks"].at[b], r["kr"].at[b], {"ep": to})

    loads["mixer_input"].wait()
    loads["mixer_gain"].wait()
    seg[t] = normalize(r["mixer_input"][...], r["mixer_gain"][...]).astype(BF16)
    pl.semaphore_wait(barrier, 2 + n_ep - 1)
    n_hi.start()
    n_lo.start()

    loads["routes"].wait()
    loads["expert_input"].wait()
    loads["expert_gain"].wait()
    experts = (n_ep + 15) // 16 * 16
    expert_ids = iota((experts, moe_rows), 0)
    chosen = [expert_ids == r["routes"][k : k + 1, :] for k in range(top_count)]
    member = functools.reduce(jnp.logical_or, chosen)
    earlier = jnp.where(iota((moe_rows, moe_rows), 0) < iota((moe_rows, moe_rows), 1), 1.0, 0.0)
    rank = jnp.dot(
        jnp.where(member, 1.0, 0.0).astype(BF16), earlier.astype(BF16), preferred_element_type=F32
    )
    slot = jnp.where(member, rank, -1.0)
    slot_rows = iota((cap, moe_rows), 0).astype(F32)
    for e in range(n_ep):
        r["dispatch"][e] = jnp.where(slot[e : e + 1, :] == slot_rows, 1.0, 0.0).astype(BF16)
    normed_moe = r["expert_input"]
    normed_moe[...] = normalize(normed_moe[...], r["expert_gain"][...]).astype(BF16)

    sent = r["dispatch"][...].reshape(n_ep * cap, moe_rows)
    out[...] = jnp.dot(sent, normed_moe[...], preferred_element_type=F32).astype(BF16).reshape(out.shape)
    if folded:
        inner = (me > 0) & (me < n_ep - 1)
        edge = jnp.logical_not(inner)
        p1 = 1 + me % 2
        p2 = jnp.where(me < 2, 2 - 2 * me, 3 - 2 * (me - 2))
        p3 = jnp.where(me < 2, 3, 0)
        copy_a(p1).start()

        @pl.when(inner)
        def _():
            copy_a(p2).start()

    else:

        @pl.loop(1, n_ep)
        def _(j):
            copy_a(lax.rem(me + j, n_ep)).start()

    rows[me, t] = out[me]
    copy_b_hi(me).start()
    copy_b_lo(me).start()

    loads["route_weight"].wait()
    weight = functools.reduce(
        lambda a, b: a + b,
        [jnp.where(chosen[k], r["route_weight"][k : k + 1, :], 0.0) for k in range(top_count)],
    )

    def turned(x):
        return jnp.concatenate([x, jnp.zeros((LANES - experts, moe_rows), F32)], axis=0).T

    slot_turned = turned(slot)
    r["weights"][...] = turned(weight)
    slot_columns = iota((moe_rows, cap), 1).astype(F32)
    for e in range(n_ep):
        r["pick"][e] = jnp.where(slot_turned[:, e : e + 1] == slot_columns, 1.0, 0.0).astype(BF16)

    def combine(e, first):
        weights = r["weights"][...]
        share = jnp.sum(jnp.where(iota(weights.shape, 1) == e, weights, 0.0), axis=1, keepdims=True)

        y = share * jnp.dot(r["pick"][e], ret[e], preferred_element_type=F32)
        r["combined"][...] = y if first else r["combined"][...] + y

    def project_in(half):
        x = seg[pl.ds(2 * half, 2)].reshape(2 * mix_rows, width)
        p = pl.ds(pl.multiple_of(half * 2 * mix_rows, 2 * mix_rows), 2 * mix_rows)
        kv[me, p, pl.ds(0, head_width)] = jnp.dot(x, wk[...], preferred_element_type=F32).astype(BF16)
        kv[me, p, pl.ds(head_width, head_width)] = jnp.dot(x, wv[...], preferred_element_type=F32).astype(BF16)
        queries[p, :] = jnp.dot(x, wq[...], preferred_element_type=F32).astype(BF16)

    def expert(s, half):
        x = rows[s, pl.ds(2 * half, 2)].reshape(2 * cap, width)
        g = jnp.dot(x, eg[...], preferred_element_type=F32)
        u = jnp.dot(x, eu[...], preferred_element_type=F32)
        hid[...] = (g / (1.0 + jnp.exp(-g)) * u).astype(BF16)
        y = jnp.dot(hid[...], ed[...], preferred_element_type=F32)
        res[s, pl.ds(2 * half, 2)] = y.astype(BF16).reshape(2, cap, width)
        copy_d(s, half).start()

    def step_e(s):
        copy_d(s, other_hi).wait_recv()
        drec[s, other_hi] = (res[s, hi_peer].astype(F32) + drec[s, other_hi].astype(F32)).astype(BF16)
        copy_e(s).start()

    def step_f(s, own):
        copy_d(s, hi).wait_recv()
        copy_e(s).wait_recv()
        total = (res[s, t].astype(F32) + drec[s, hi].astype(F32) + erec[s].astype(F32)).astype(BF16)
        if own:
            ret[s] = total
        else:
            copy_a(s).wait_send()
            fin[s] = total
            copy_f(s).start()

    scale = head_dim ** (-0.5) * LOG2_E

    def block(b):
        return pl.ds(pl.multiple_of(b * span, span), span)

    def attend(q, qb, b, cols, i, masked, first):
        for h in range(heads):
            hc = pl.ds(h * head_dim, head_dim)
            vc = pl.ds(head_width + h * head_dim, head_dim)
            s = lax.dot_general(kv[b, :, hc], q[:, hc], (((1,), (1,)), ((), ())), preferred_element_type=F32)
            s = s * scale + (gate[h : h + 1, block(qb)] - cols[:, h : h + 1])
            if masked:
                s = jnp.where(iota(s.shape, 0) <= iota(s.shape, 1), s, MASKED)
            new = jnp.max(s, axis=0, keepdims=True)
            if not first:
                old = run_max[i, h : h + 1]
                new = jnp.maximum(old, new)
                fix = jnp.exp2(old - new)
            w = jnp.exp2(s - new)
            part_sum = jnp.sum(w, axis=0, keepdims=True)
            part_acc = lax.dot_general(
                kv[b, :, vc], w.astype(BF16), (((0,), (0,)), ((), ())), preferred_element_type=F32
            )
            run_max[i, h : h + 1] = new
            if first:
                run_sum[i, h : h + 1] = part_sum
                run_acc[i, h] = part_acc
            else:
                run_sum[i, h : h + 1] = run_sum[i, h : h + 1] * fix + part_sum
                run_acc[i, h] = run_acc[i, h] * fix + part_acc

    def finish():
        for h in range(heads):
            mean = run_acc[0, h] / run_sum[0, h : h + 1]
            attended[:, pl.ds(h * head_dim, head_dim)] = mean.T.astype(BF16)

    def load_gate():
        loads["gate"].wait()
        gate[...] = gate[...] * LOG2_E

    def gate_columns(i, b):
        columns[i] = columns_of(gate[:, block(b)])

    part = seg

    def project(b):
        x = attended[pl.ds(pl.multiple_of(b * mix_rows, mix_rows), mix_rows), :]

        part[b] = jnp.dot(x, wo[...], preferred_element_type=F32).astype(BF16)

    def copy_m(h):
        return remote(part.at[2 * h + (1 - lo)], mdrec.at[h], r["ms"].at[h], r["mr"].at[h], {"tp": lo_peer})

    m_hi = remote(mdrec.at[other_hi], merec, r["ms"].at[2], r["mr"].at[2], {"tp": hi_peer})

    def mix_out():
        loads["wo"].wait()
        n_hi.wait_send()
        n_lo.wait_send()
        n_relay.wait_send()
        project(diag_peer)
        copy_m(other_hi).start()
        project(hi_peer)
        copy_m(other_hi).wait_recv()
        mdrec[other_hi] = (part[hi_peer].astype(F32) + mdrec[other_hi].astype(F32)).astype(BF16)
        m_hi.start()
        project(lo_peer)
        copy_m(hi).start()
        project(t)

    def mix_end():
        copy_m(hi).wait_recv()
        loads["post_gain"].wait()
        m_hi.wait_recv()
        total = part[t].astype(F32) + mdrec[hi].astype(F32) + merec[...].astype(F32)
        inverse = lax.rsqrt(jnp.mean(total * total, axis=-1, keepdims=True) + EPS)
        r["mixer_out"][...] = (total * inverse * r["post_gain"][...]).astype(BF16)

    def relay_b(s):
        recv_a(s).wait_recv()
        copy_b_hi(s).start()
        copy_b_lo(s).start()

    def relay_c(s):
        copy_b_hi(s).wait_recv()
        copy_c(s).start()

    def expert_own(s):
        copy_b_lo(s).wait_recv()
        expert(s, hi)

    def expert_other(s):
        copy_c(s).wait_recv()
        expert(s, other_hi)

    if folded:
        qin, obuf, lbuf, oin, lin = r["qin"], r["obuf"], r["lbuf"], r["oin"], r["lin"]
        first, second, helper, last = me == 0, me == 1, me == 2, me == 3
        copy_q = remote(queries, qin, r["qs"].at[0], r["qr"].at[0], {"ep": 2})
        copy_o = remote(obuf, oin, r["os"].at[0], r["or"].at[0], {"ep": 3})
        copy_l = remote(lbuf, lin, r["os"].at[1], r["or"].at[1], {"ep": 3})

        for name in ("wq", "wk", "wv"):
            loads[name].wait()
        n_lo.wait_recv()
        project_in(hi)
        for name in ("eg", "eu", "ed"):
            loads[name].wait()
        expert_own(me)
        load_gate()
        gate_columns(0, me)

        @pl.when(inner)
        def _():
            gate_columns(1, me - 1)

        @pl.when(helper)
        def _():
            gate_columns(2, 0)

        relay_b(p1)

        @pl.when(inner)
        def _():
            relay_b(p2)

        @pl.when(edge)
        def _():
            copy_a(p2).start()

        copy_a(p3).start()
        n_hi.wait_recv()
        n_relay.start()
        expert_own(p1)
        n_relay.wait_recv()
        project_in(other_hi)

        @pl.when(first)
        def _():
            copy_kv(0, 1).start()

        @pl.when(last)
        def _():
            copy_q.start()

        attend(queries, me, me, columns.at[0], 0, True, True)
        relay_c(me)
        expert_other(me)

        @pl.when(second)
        def _():
            copy_kv(1, 2).start()

        @pl.when(inner)
        def _():
            expert_own(p2)

        @pl.when(edge)
        def _():
            step_e(me)

        relay_c(p1)
        expert_other(p1)
        step_e(p1)

        @pl.when(edge)
        def _():
            relay_b(p2)

        relay_b(p3)

        @pl.when(edge)
        def _():
            expert_own(p2)

        @pl.when(helper)
        def _():
            copy_q.wait_recv()
            attend(qin, 3, 2, columns.at[0], 1, False, True)

        expert_own(p3)

        @pl.when(second)
        def _():
            copy_kv(0, 1).wait_recv()
            copy_kv(0, 2).start()
            attend(queries, 1, 0, columns.at[1], 0, False, False)

        relay_c(p2)
        expert_other(p2)
        step_e(p2)

        @pl.when(helper)
        def _():
            copy_kv(1, 2).wait_recv()
            attend(queries, 2, 1, columns.at[1], 0, False, False)
            attend(qin, 3, 1, columns.at[1], 1, False, False)

        relay_c(p3)
        expert_other(p3)
        step_e(p3)

        @pl.when(inner)
        def _():
            step_e(me)

        step_f(p1, False)

        @pl.when(helper)
        def _():
            copy_kv(0, 2).wait_recv()
            attend(qin, 3, 0, columns.at[2], 1, False, False)
            for h in range(heads):
                total = run_sum[1, h : h + 1]
                obuf[pl.ds(h * head_dim, head_dim)] = (run_acc[1, h] / total).astype(BF16)
                lbuf[h : h + 1] = run_max[1, h : h + 1] + jnp.log2(total)
            copy_o.start()
            copy_l.start()
            attend(queries, 2, 0, columns.at[2], 0, False, False)

        step_f(p2, False)

        @pl.when(jnp.logical_not(last))
        def _():
            finish()

        @pl.when(last)
        def _():
            copy_o.wait_recv()
            copy_l.wait_recv()
            for h in range(heads):
                hc = pl.ds(h * head_dim, head_dim)
                far, old = lin[h : h + 1], run_max[0, h : h + 1]
                new = jnp.maximum(old, far)
                fix, far_fix = jnp.exp2(old - new), jnp.exp2(far - new)
                numer = run_acc[0, h] * fix + oin[hc].astype(F32) * far_fix
                attended[:, hc] = (numer / (run_sum[0, h : h + 1] * fix + far_fix)).T.astype(BF16)

        mix_out()
        step_f(p3, False)
        step_f(me, True)
        combine(me, True)
        for e in (p1, p2, p3):
            recv_f(e).wait_recv()
            combine(e, False)
        r["expert_out"][...] = r["combined"][...].astype(BF16)
        mix_end()

        @pl.when(first)
        def _():
            copy_kv(0, 1).wait_send()

        @pl.when(second)
        def _():
            copy_kv(1, 2).wait_send()
            copy_kv(0, 2).wait_send()

        @pl.when(helper)
        def _():
            copy_o.wait_send()
            copy_l.wait_send()

        @pl.when(last)
        def _():
            copy_q.wait_send()

    else:
        step = lambda j: lax.rem(me + j, n_ep)
        for name in ("wq", "wk", "wv"):
            loads[name].wait()
        n_hi.wait_recv()
        n_relay.start()
        n_lo.wait_recv()
        project_in(hi)
        n_relay.wait_recv()
        project_in(other_hi)

        @pl.when(me + 1 < n_ep)
        def _():
            copy_kv(me, me + 1).start()

        for name in ("eg", "eu", "ed"):
            loads[name].wait()
        load_gate()
        gate_columns(0, me)

        @pl.loop(0, n_ep)
        def _(j):
            s = step(j)

            @pl.when(j + 1 < n_ep)
            def _():
                relay_b(step(j + 1))

            expert_own(s)
            relay_c(s)
            expert_other(s)

            @pl.when(j >= 1)
            def _():
                step_e(step(j - 1))

            @pl.when((j >= 1) & (j < n_ep - 1) & (me - j >= 0))
            def _():
                copy_kv(me - j, me).wait_recv()

                @pl.when(me + 1 < n_ep)
                def _():
                    copy_kv(me - j, me + 1).start()

        step_e(step(n_ep - 1))
        attend(queries, me, me, columns.at[0], 0, True, True)
        step_f(me, True)
        combine(me, True)

        @pl.loop(1, n_ep)
        def _(j):
            step_f(step(j), False)

        @pl.loop(1, me + 1)
        def _(d):
            @pl.when(d == n_ep - 1)
            def _():
                copy_kv(0, me).wait_recv()

            gate_columns(0, me - d)
            attend(queries, me, me - d, columns.at[0], 0, False, False)

        finish()
        mix_out()

        @pl.loop(1, n_ep)
        def _(j):
            recv_f(step(j)).wait_recv()
            combine(step(j), False)

        r["expert_out"][...] = r["combined"][...].astype(BF16)
        mix_end()

        @pl.when(me + 1 < n_ep)
        def _():
            @pl.loop(0, me + 1)
            def _(b):
                copy_kv(b, me + 1).wait_send()

    copy_m(0).wait_send()
    copy_m(1).wait_send()
    m_hi.wait_send()

    @pl.loop(0, n_ep)
    def _(j):
        s = lax.rem(me + j, n_ep)

        @pl.when(j > 0)
        def _():
            copy_f(s).wait_send()

        copy_b_hi(s).wait_send()
        copy_b_lo(s).wait_send()
        copy_c(s).wait_send()
        copy_d(s, 0).wait_send()
        copy_d(s, 1).wait_send()
        copy_e(s).wait_send()


def hand_out(*refs):
    sources, places, held, sems = refs[:2], refs[2:4], refs[4:6], refs[6]
    half = held[0].shape[0] // 2
    loads, stores = [], []
    for i, (source, place, part) in enumerate(zip(sources, places, held)):
        for k in range(2):
            p = pl.ds(k * half, half)
            loads.append(pltpu.make_async_copy(source.at[p], part.at[p], sems.at[0, 2 * i + k]))
            stores.append(pltpu.make_async_copy(part.at[p], place.at[p], sems.at[1, 2 * i + k]))
    for load in loads:
        load.start()
    for load, store in zip(loads, stores):
        load.wait()
        store.start()
    for store in stores:
        store.wait()


def on_device(
    mixer_input,
    forget_cumsum,
    mixer_gain,
    query_weight,
    key_weight,
    value_weight,
    out_weight,
    post_gain,
    expert_input,
    expert_gain,
    routes,
    route_weight,
    expert_gate,
    expert_upward,
    expert_down,
):
    n_ep = lax.axis_size("ep")
    n_tp = lax.axis_size("tp")
    mix_rows, width = mixer_input.shape
    heads = forget_cumsum.shape[0]
    head_width = query_weight.shape[1]
    head_dim = head_width // heads
    span = mix_rows * n_tp
    moe_rows, top_count = routes.shape
    assert n_tp == 4 and expert_gate.shape[0] == 1
    capacity = (moe_rows * top_count * 9 + 8 * n_ep - 1) // (8 * n_ep)
    cap = (capacity + ROW_TILE - 1) // ROW_TILE * ROW_TILE
    f_width = expert_gate.shape[2]
    folded = n_ep == 4
    sets = 2 if folded else 1

    inputs = {
        "mixer_input": mixer_input,
        "mixer_gain": mixer_gain.reshape(1, -1),
        "routes": routes.T,
        "expert_input": expert_input,
        "expert_gain": expert_gain.reshape(1, -1),
        "wq": query_weight,
        "wk": key_weight,
        "wv": value_weight,
        "eg": expert_gate[0],
        "eu": expert_upward[0],
        "ed": expert_down[0],
        "route_weight": route_weight.T,
        "gate": forget_cumsum,
        "post_gain": post_gain.reshape(1, -1),
        "wo": out_weight,
    }
    vmem, dma = pltpu.VMEM, pltpu.SemaphoreType.DMA
    scratch = {name: vmem(x.shape, x.dtype) for name, x in inputs.items()}
    scratch |= {
        "seg": vmem((4, mix_rows, width), BF16),
        "queries": vmem((span, head_width), BF16),
        "kv": vmem((n_ep, span, 2 * head_width), BF16),
        "rows": vmem((n_ep, 4, cap, width), BF16),
        "out": vmem((n_ep, cap, width), BF16),
        "dispatch": vmem((n_ep, cap, moe_rows), BF16),
        "pick": vmem((n_ep, moe_rows, cap), BF16),
        "weights": vmem((moe_rows, LANES), F32),
        "combined": vmem((moe_rows, width), F32),
        "hid": vmem((2 * cap, f_width), BF16),
        "res": vmem((n_ep, 4, cap, width), BF16),
        "drec": vmem((n_ep, 2, cap, width), BF16),
        "erec": vmem((n_ep, cap, width), BF16),
        "ret": vmem((n_ep, cap, width), BF16),
        "run_max": vmem((sets, heads, span), F32),
        "run_sum": vmem((sets, heads, span), F32),
        "run_acc": vmem((sets, heads, head_dim, span), F32),
        "attended": vmem((span, head_width), BF16),
        "columns": vmem((3 if folded else 1, span, LANES), F32),
        "mdrec": vmem((2, mix_rows, width), BF16),
        "load_sem": dma((len(inputs),)),
    }
    if folded:
        scratch |= {
            "qin": vmem((span, head_width), BF16),
            "obuf": vmem((head_width, span), BF16),
            "lbuf": vmem((8, span), F32),
            "oin": vmem((head_width, span), BF16),
            "lin": vmem((8, span), F32),
            "qs": dma((1,)),
            "qr": dma((1,)),
            "os": dma((2,)),
            "or": dma((2,)),
        }
    scratch |= {"ns": dma((3,)), "nr": dma((3,)), "ms": dma((3,)), "mr": dma((3,))}
    for name in ("a", "c", "e", "f", "k"):
        scratch |= {name + "s": dma((n_ep,)), name + "r": dma((n_ep,))}
    for name in ("b", "d"):
        scratch |= {name + "s": dma((2, n_ep)), name + "r": dma((2, n_ep))}

    labels = [name + "_hbm" for name in inputs] + ["mixer_out", "expert_out"] + list(scratch)

    def body(*refs):
        kernel(n_ep, head_dim, dict(zip(labels, refs, strict=True)))

    block = pl.BlockSpec(memory_space=pltpu.VMEM)
    results = pl.pallas_call(
        body,
        out_shape=(
            jax.ShapeDtypeStruct((mix_rows, width), BF16),
            jax.ShapeDtypeStruct((moe_rows, width), BF16),
        ),
        in_specs=[pl.BlockSpec(memory_space=pl.ANY)] * len(inputs),
        out_specs=(block, block),
        scratch_shapes=list(scratch.values()),
        compiler_params=pltpu.CompilerParams(
            collective_id=0, has_side_effects=True, vmem_limit_bytes=66_500_000
        ),
    )(*inputs.values())
    anywhere = pl.BlockSpec(memory_space=pl.ANY)
    return pl.pallas_call(
        hand_out,
        out_shape=tuple(jax.ShapeDtypeStruct(x.shape, x.dtype) for x in results),
        in_specs=[anywhere] * 2,
        out_specs=(anywhere,) * 2,
        scratch_shapes=[vmem(x.shape, x.dtype) for x in results] + [dma((2, 4))],
    )(*results)


def solution(mesh):
    rows = P(("grp", "ep", "tp"), None)
    in_specs = (
        rows,
        P("tp", "grp"),
        P(),
        P(None, "tp"),
        P(None, "tp"),
        P(None, "tp"),
        P("tp", None),
        P(),
        rows,
        P(),
        rows,
        rows,
        P("ep", None, "tp"),
        P("ep", None, "tp"),
        P("ep", "tp", None),
    )
    return jax.shard_map(
        on_device, mesh=mesh, in_specs=in_specs, out_specs=(rows, rows), check_vma=False
    )
```

```python
import functools

import jax
import jax.numpy as jnp
from jax import lax
from jax.experimental import pallas as pl
from jax.experimental.pallas import tpu as pltpu
from jax.sharding import PartitionSpec as P

EPS = 1e-06
MASKED = -1e30
MESH = pl.DeviceIdType.MESH
F32 = jnp.float32
BF16 = jnp.bfloat16
ROW_TILE = 8
LANES = 128
LOG2_E = 1.4426950408889634


def normalize(row_block, gain):
    values = row_block.astype(F32)
    inverse = lax.rsqrt(jnp.mean(values * values, axis=-1, keepdims=True) + EPS)
    return values * inverse * gain


def iota(shape, dim):
    return lax.broadcasted_iota(jnp.int32, shape, dim)


def columns_of(rows):
    spread = jnp.broadcast_to(rows[0:1], (LANES, rows.shape[1]))
    which = iota(spread.shape, 0)
    for h in range(1, rows.shape[0]):
        spread = jnp.where(which == h, rows[h : h + 1], spread)
    return spread.T


def kernel(
    n_ep,
    head_dim,
    refs,
):
    r = refs
    me = lax.axis_index("ep")
    t = lax.axis_index("tp")
    hi = t // 2
    lo = t % 2
    lo_peer = 2 * hi + (1 - lo)
    hi_peer = 2 * (1 - hi) + lo
    other_hi = 1 - hi
    seg, queries, kv, rows, out = r["seg"], r["queries"], r["kv"], r["rows"], r["out"]
    hid, res, drec, erec, fin, ret = r["hid"], r["res"], r["drec"], r["erec"], out, r["ret"]
    run_max, run_sum, run_acc, attended = r["run_max"], r["run_sum"], r["run_acc"], r["attended"]
    mdrec, merec, gate, columns = r["mdrec"], r["mixer_input"], r["gate"], r["columns"]
    wq, wk, wv, wo, eg, eu, ed = (r[k] for k in ("wq", "wk", "wv", "wo", "eg", "eu", "ed"))
    mix_rows, width = r["mixer_out"].shape
    head_width = wq.shape[1]
    heads = head_width // head_dim
    span = 4 * mix_rows
    cap = out.shape[1]
    top_count, moe_rows = r["routes"].shape
    folded = n_ep == 4

    def remote(src, dst, send_sem, recv_sem, where):
        return pltpu.make_async_remote_copy(
            src_ref=src,
            dst_ref=dst,
            send_sem=send_sem,
            recv_sem=recv_sem,
            device_id=where,
            device_id_type=MESH,
        )

    names = (
        "mixer_input", "mixer_gain", "routes", "expert_input", "expert_gain", "wq", "wk", "wv",
        "eg", "eu", "ed", "route_weight", "gate", "post_gain", "wo",
    )
    loads = {
        name: pltpu.make_async_copy(r[name + "_hbm"], r[name], r["load_sem"].at[i])
        for i, name in enumerate(names)
    }
    barrier = pltpu.get_barrier_semaphore()
    pl.semaphore_signal(barrier, inc=1, device_id={"tp": lo_peer}, device_id_type=MESH)
    pl.semaphore_signal(barrier, inc=1, device_id={"tp": hi_peer}, device_id_type=MESH)

    @pl.loop(1, n_ep)
    def _(j):
        pl.semaphore_signal(barrier, inc=1, device_id={"ep": lax.rem(me + j, n_ep)}, device_id_type=MESH)

    for name in names:
        loads[name].start()

    n_hi = remote(seg.at[t], seg.at[t], r["ns"].at[0], r["nr"].at[0], {"tp": hi_peer})
    n_lo = remote(seg.at[t], seg.at[t], r["ns"].at[1], r["nr"].at[1], {"tp": lo_peer})
    n_relay = remote(seg.at[hi_peer], seg.at[hi_peer], r["ns"].at[2], r["nr"].at[2], {"tp": lo_peer})
    diag_peer = 2 * other_hi + (1 - lo)

    def copy_a(to):
        return remote(out.at[to], rows.at[me, t], r["as"].at[to], r["ar"].at[me], {"ep": to})

    def recv_a(s):
        return remote(out.at[s], rows.at[s, t], r["as"].at[s], r["ar"].at[s], {"ep": s})

    def copy_b_hi(s):
        return remote(rows.at[s, t], rows.at[s, t], r["bs"].at[0, s], r["br"].at[0, s], {"tp": hi_peer})

    def copy_b_lo(s):
        return remote(rows.at[s, t], rows.at[s, t], r["bs"].at[1, s], r["br"].at[1, s], {"tp": lo_peer})

    def copy_c(s):
        return remote(rows.at[s, hi_peer], rows.at[s, hi_peer], r["cs"].at[s], r["cr"].at[s], {"tp": lo_peer})

    def copy_d(s, h):
        return remote(res.at[s, 2 * h + (1 - lo)], drec.at[s, h], r["ds"].at[h, s], r["dr"].at[h, s], {"tp": lo_peer})

    def copy_e(s):
        return remote(drec.at[s, other_hi], erec.at[s], r["es"].at[s], r["er"].at[s], {"tp": hi_peer})

    def copy_f(s):
        return remote(fin.at[s], ret.at[me], r["fs"].at[s], r["fr"].at[me], {"ep": s})

    def recv_f(e):
        return remote(fin.at[e], ret.at[e], r["fs"].at[e], r["fr"].at[e], {"ep": e})

    def copy_kv(b, to):
        return remote(kv.at[b], kv.at[b], r["ks"].at[b], r["kr"].at[b], {"ep": to})

    loads["mixer_input"].wait()
    loads["mixer_gain"].wait()
    seg[t] = normalize(r["mixer_input"][...], r["mixer_gain"][...]).astype(BF16)
    pl.semaphore_wait(barrier, 2 + n_ep - 1)
    n_hi.start()
    n_lo.start()

    loads["routes"].wait()
    loads["expert_input"].wait()
    loads["expert_gain"].wait()
    experts = (n_ep + 15) // 16 * 16
    expert_ids = iota((experts, moe_rows), 0)
    chosen = [expert_ids == r["routes"][k : k + 1, :] for k in range(top_count)]
    member = functools.reduce(jnp.logical_or, chosen)
    earlier = jnp.where(iota((moe_rows, moe_rows), 0) < iota((moe_rows, moe_rows), 1), 1.0, 0.0)
    rank = jnp.dot(
        jnp.where(member, 1.0, 0.0).astype(BF16), earlier.astype(BF16), preferred_element_type=F32
    )
    slot = jnp.where(member, rank, -1.0)
    slot_rows = iota((cap, moe_rows), 0).astype(F32)
    for e in range(n_ep):
        r["dispatch"][e] = jnp.where(slot[e : e + 1, :] == slot_rows, 1.0, 0.0).astype(BF16)
    normed_moe = r["expert_input"]
    normed_moe[...] = normalize(normed_moe[...], r["expert_gain"][...]).astype(BF16)

    sent = r["dispatch"][...].reshape(n_ep * cap, moe_rows)
    out[...] = jnp.dot(sent, normed_moe[...], preferred_element_type=F32).astype(BF16).reshape(out.shape)
    if folded:
        inner = (me > 0) & (me < n_ep - 1)
        edge = jnp.logical_not(inner)
        p1 = 1 + me % 2
        p2 = jnp.where(me < 2, 2 - 2 * me, 3 - 2 * (me - 2))
        p3 = jnp.where(me < 2, 3, 0)
        copy_a(p1).start()

        @pl.when(inner)
        def _():
            copy_a(p2).start()

    else:

        @pl.loop(1, n_ep)
        def _(j):
            copy_a(lax.rem(me + j, n_ep)).start()

    rows[me, t] = out[me]
    copy_b_hi(me).start()
    copy_b_lo(me).start()

    loads["route_weight"].wait()
    weight = functools.reduce(
        lambda a, b: a + b,
        [jnp.where(chosen[k], r["route_weight"][k : k + 1, :], 0.0) for k in range(top_count)],
    )

    def turned(x):
        return jnp.concatenate([x, jnp.zeros((LANES - experts, moe_rows), F32)], axis=0).T

    slot_turned = turned(slot)
    r["weights"][...] = turned(weight)
    slot_columns = iota((moe_rows, cap), 1).astype(F32)
    for e in range(n_ep):
        r["pick"][e] = jnp.where(slot_turned[:, e : e + 1] == slot_columns, 1.0, 0.0).astype(BF16)

    def combine(e, first):
        weights = r["weights"][...]
        share = jnp.sum(jnp.where(iota(weights.shape, 1) == e, weights, 0.0), axis=1, keepdims=True)

        y = share * jnp.dot(r["pick"][e], ret[e], preferred_element_type=F32)
        r["combined"][...] = y if first else r["combined"][...] + y

    def project_in(half):
        x = seg[pl.ds(2 * half, 2)].reshape(2 * mix_rows, width)
        p = pl.ds(pl.multiple_of(half * 2 * mix_rows, 2 * mix_rows), 2 * mix_rows)
        kv[me, p, pl.ds(0, head_width)] = jnp.dot(x, wk[...], preferred_element_type=F32).astype(BF16)
        kv[me, p, pl.ds(head_width, head_width)] = jnp.dot(x, wv[...], preferred_element_type=F32).astype(BF16)
        queries[p, :] = jnp.dot(x, wq[...], preferred_element_type=F32).astype(BF16)

    def expert(s, half):
        x = rows[s, pl.ds(2 * half, 2)].reshape(2 * cap, width)
        g = jnp.dot(x, eg[...], preferred_element_type=F32)
        u = jnp.dot(x, eu[...], preferred_element_type=F32)
        hid[...] = (g / (1.0 + jnp.exp(-g)) * u).astype(BF16)
        y = jnp.dot(hid[...], ed[...], preferred_element_type=F32)
        res[s, pl.ds(2 * half, 2)] = y.astype(BF16).reshape(2, cap, width)
        copy_d(s, half).start()

    def step_e(s):
        copy_d(s, other_hi).wait_recv()
        drec[s, other_hi] = (res[s, hi_peer].astype(F32) + drec[s, other_hi].astype(F32)).astype(BF16)
        copy_e(s).start()

    def step_f(s, own):
        copy_d(s, hi).wait_recv()
        copy_e(s).wait_recv()
        total = (res[s, t].astype(F32) + drec[s, hi].astype(F32) + erec[s].astype(F32)).astype(BF16)
        if own:
            ret[s] = total
        else:
            copy_a(s).wait_send()
            fin[s] = total
            copy_f(s).start()

    scale = head_dim ** (-0.5) * LOG2_E

    def block(b):
        return pl.ds(pl.multiple_of(b * span, span), span)

    def attend(q, qb, b, cols, i, masked, first):
        for h in range(heads):
            hc = pl.ds(h * head_dim, head_dim)
            vc = pl.ds(head_width + h * head_dim, head_dim)
            s = lax.dot_general(kv[b, :, hc], q[:, hc], (((1,), (1,)), ((), ())), preferred_element_type=F32)
            s = s * scale + (gate[h : h + 1, block(qb)] - cols[:, h : h + 1])
            if masked:
                s = jnp.where(iota(s.shape, 0) <= iota(s.shape, 1), s, MASKED)
            new = jnp.max(s, axis=0, keepdims=True)
            if not first:
                old = run_max[i, h : h + 1]
                new = jnp.maximum(old, new)
                fix = jnp.exp2(old - new)
            w = jnp.exp2(s - new)
            part_sum = jnp.sum(w, axis=0, keepdims=True)
            part_acc = lax.dot_general(
                kv[b, :, vc], w.astype(BF16), (((0,), (0,)), ((), ())), preferred_element_type=F32
            )
            run_max[i, h : h + 1] = new
            if first:
                run_sum[i, h : h + 1] = part_sum
                run_acc[i, h] = part_acc
            else:
                run_sum[i, h : h + 1] = run_sum[i, h : h + 1] * fix + part_sum
                run_acc[i, h] = run_acc[i, h] * fix + part_acc

    def finish():
        for h in range(heads):
            mean = run_acc[0, h] / run_sum[0, h : h + 1]
            attended[:, pl.ds(h * head_dim, head_dim)] = mean.T.astype(BF16)

    def load_gate():
        loads["gate"].wait()
        gate[...] = gate[...] * LOG2_E

    def gate_columns(i, b):
        columns[i] = columns_of(gate[:, block(b)])

    part = seg

    def project(b):
        x = attended[pl.ds(pl.multiple_of(b * mix_rows, mix_rows), mix_rows), :]

        part[b] = jnp.dot(x, wo[...], preferred_element_type=F32).astype(BF16)

    def copy_m(h):
        return remote(part.at[2 * h + (1 - lo)], mdrec.at[h], r["ms"].at[h], r["mr"].at[h], {"tp": lo_peer})

    m_hi = remote(mdrec.at[other_hi], merec, r["ms"].at[2], r["mr"].at[2], {"tp": hi_peer})

    def mix_out():
        loads["wo"].wait()
        n_hi.wait_send()
        n_lo.wait_send()
        n_relay.wait_send()
        project(diag_peer)
        copy_m(other_hi).start()
        project(hi_peer)
        copy_m(other_hi).wait_recv()
        mdrec[other_hi] = (part[hi_peer].astype(F32) + mdrec[other_hi].astype(F32)).astype(BF16)
        m_hi.start()
        project(lo_peer)
        copy_m(hi).start()
        project(t)

    def mix_end():
        copy_m(hi).wait_recv()
        loads["post_gain"].wait()
        m_hi.wait_recv()
        total = part[t].astype(F32) + mdrec[hi].astype(F32) + merec[...].astype(F32)
        inverse = lax.rsqrt(jnp.mean(total * total, axis=-1, keepdims=True) + EPS)
        r["mixer_out"][...] = (total * inverse * r["post_gain"][...]).astype(BF16)

    def relay_b(s):
        recv_a(s).wait_recv()
        copy_b_hi(s).start()
        copy_b_lo(s).start()

    def relay_c(s):
        copy_b_hi(s).wait_recv()
        copy_c(s).start()

    def expert_own(s):
        copy_b_lo(s).wait_recv()
        expert(s, hi)

    def expert_other(s):
        copy_c(s).wait_recv()
        expert(s, other_hi)

    if folded:
        qin, obuf, lbuf, oin, lin = r["qin"], r["obuf"], r["lbuf"], r["oin"], r["lin"]
        first, second, helper, last = me == 0, me == 1, me == 2, me == 3
        copy_q = remote(queries, qin, r["qs"].at[0], r["qr"].at[0], {"ep": 2})
        copy_o = remote(obuf, oin, r["os"].at[0], r["or"].at[0], {"ep": 3})
        copy_l = remote(lbuf, lin, r["os"].at[1], r["or"].at[1], {"ep": 3})

        for name in ("wq", "wk", "wv"):
            loads[name].wait()
        n_lo.wait_recv()
        project_in(hi)
        for name in ("eg", "eu", "ed"):
            loads[name].wait()
        expert_own(me)
        load_gate()
        gate_columns(0, me)

        @pl.when(inner)
        def _():
            gate_columns(1, me - 1)

        @pl.when(helper)
        def _():
            gate_columns(2, 0)

        relay_b(p1)

        @pl.when(inner)
        def _():
            relay_b(p2)

        @pl.when(edge)
        def _():
            copy_a(p2).start()

        copy_a(p3).start()
        n_hi.wait_recv()
        n_relay.start()
        expert_own(p1)
        n_relay.wait_recv()
        project_in(other_hi)

        @pl.when(first)
        def _():
            copy_kv(0, 1).start()

        @pl.when(last)
        def _():
            copy_q.start()

        attend(queries, me, me, columns.at[0], 0, True, True)
        relay_c(me)
        expert_other(me)

        @pl.when(second)
        def _():
            copy_kv(1, 2).start()

        @pl.when(inner)
        def _():
            expert_own(p2)

        @pl.when(edge)
        def _():
            step_e(me)

        relay_c(p1)
        expert_other(p1)

        @pl.when(jnp.logical_not(last))
        def _():
            step_e(p1)

        @pl.when(edge)
        def _():
            relay_b(p2)

        relay_b(p3)

        @pl.when(edge)
        def _():
            expert_own(p2)

        @pl.when(helper)
        def _():
            copy_q.wait_recv()
            attend(qin, 3, 2, columns.at[0], 1, False, True)

        expert_own(p3)

        @pl.when(second)
        def _():
            copy_kv(0, 1).wait_recv()
            copy_kv(0, 2).start()
            attend(queries, 1, 0, columns.at[1], 0, False, False)

        relay_c(p2)
        expert_other(p2)
        step_e(p2)

        @pl.when(helper)
        def _():
            copy_kv(1, 2).wait_recv()
            attend(queries, 2, 1, columns.at[1], 0, False, False)
            attend(qin, 3, 1, columns.at[1], 1, False, False)

        relay_c(p3)
        expert_other(p3)
        step_e(p3)

        @pl.when(inner)
        def _():
            step_e(me)

        @pl.when(last)
        def _():
            step_e(p1)

        @pl.when(jnp.logical_not(last))
        def _():
            step_f(p1, False)

        @pl.when(helper)
        def _():
            copy_kv(0, 2).wait_recv()
            attend(qin, 3, 0, columns.at[2], 1, False, False)
            for h in range(heads):
                total = run_sum[1, h : h + 1]
                obuf[pl.ds(h * head_dim, head_dim)] = (run_acc[1, h] / total).astype(BF16)
                lbuf[h : h + 1] = run_max[1, h : h + 1] + jnp.log2(total)
            copy_o.start()
            copy_l.start()
            attend(queries, 2, 0, columns.at[2], 0, False, False)

        @pl.when(jnp.logical_not(helper))
        def _():
            step_f(p2, False)

        @pl.when(jnp.logical_not(last))
        def _():
            finish()

        @pl.when(last)
        def _():
            step_f(p3, False)
            copy_o.wait_recv()
            copy_l.wait_recv()
            for h in range(heads):
                hc = pl.ds(h * head_dim, head_dim)
                far, old = lin[h : h + 1], run_max[0, h : h + 1]
                new = jnp.maximum(old, far)
                fix, far_fix = jnp.exp2(old - new), jnp.exp2(far - new)
                numer = run_acc[0, h] * fix + oin[hc].astype(F32) * far_fix
                attended[:, hc] = (numer / (run_sum[0, h : h + 1] * fix + far_fix)).T.astype(BF16)

        mix_out()

        step_f(jnp.where(last, p1, p3), False)

        @pl.when(helper)
        def _():
            copy_o.wait_send()
            copy_l.wait_send()
            step_f(p2, False)

        step_f(me, True)

        combine(me, True)
        for e in (p1, p2, p3):
            recv_f(e).wait_recv()
            combine(e, False)
        r["expert_out"][...] = r["combined"][...].astype(BF16)
        mix_end()

        @pl.when(first)
        def _():
            copy_kv(0, 1).wait_send()

        @pl.when(second)
        def _():
            copy_kv(1, 2).wait_send()
            copy_kv(0, 2).wait_send()

        @pl.when(last)
        def _():
            copy_q.wait_send()

    else:
        step = lambda j: lax.rem(me + j, n_ep)
        for name in ("wq", "wk", "wv"):
            loads[name].wait()
        n_hi.wait_recv()
        n_relay.start()
        n_lo.wait_recv()
        project_in(hi)
        n_relay.wait_recv()
        project_in(other_hi)

        @pl.when(me + 1 < n_ep)
        def _():
            copy_kv(me, me + 1).start()

        for name in ("eg", "eu", "ed"):
            loads[name].wait()
        load_gate()
        gate_columns(0, me)

        @pl.loop(0, n_ep)
        def _(j):
            s = step(j)

            @pl.when(j + 1 < n_ep)
            def _():
                relay_b(step(j + 1))

            expert_own(s)
            relay_c(s)
            expert_other(s)

            @pl.when(j >= 1)
            def _():
                step_e(step(j - 1))

            @pl.when((j >= 1) & (j < n_ep - 1) & (me - j >= 0))
            def _():
                copy_kv(me - j, me).wait_recv()

                @pl.when(me + 1 < n_ep)
                def _():
                    copy_kv(me - j, me + 1).start()

        step_e(step(n_ep - 1))
        attend(queries, me, me, columns.at[0], 0, True, True)
        step_f(me, True)
        combine(me, True)

        @pl.loop(1, n_ep)
        def _(j):
            step_f(step(j), False)

        @pl.loop(1, me + 1)
        def _(d):
            @pl.when(d == n_ep - 1)
            def _():
                copy_kv(0, me).wait_recv()

            gate_columns(0, me - d)
            attend(queries, me, me - d, columns.at[0], 0, False, False)

        finish()
        mix_out()

        @pl.loop(1, n_ep)
        def _(j):
            recv_f(step(j)).wait_recv()
            combine(step(j), False)

        r["expert_out"][...] = r["combined"][...].astype(BF16)
        mix_end()

        @pl.when(me + 1 < n_ep)
        def _():
            @pl.loop(0, me + 1)
            def _(b):
                copy_kv(b, me + 1).wait_send()

    copy_m(0).wait_send()
    copy_m(1).wait_send()
    m_hi.wait_send()

    @pl.loop(0, n_ep)
    def _(j):
        s = lax.rem(me + j, n_ep)

        @pl.when(j > 0)
        def _():
            copy_f(s).wait_send()

        copy_b_hi(s).wait_send()
        copy_b_lo(s).wait_send()
        copy_c(s).wait_send()
        copy_d(s, 0).wait_send()
        copy_d(s, 1).wait_send()
        copy_e(s).wait_send()


def hand_out(*refs):
    sources, places, held, sems = refs[:2], refs[2:4], refs[4:6], refs[6]
    half = held[0].shape[0] // 2
    loads, stores = [], []
    for i, (source, place, part) in enumerate(zip(sources, places, held)):
        for k in range(2):
            p = pl.ds(k * half, half)
            loads.append(pltpu.make_async_copy(source.at[p], part.at[p], sems.at[0, 2 * i + k]))
            stores.append(pltpu.make_async_copy(part.at[p], place.at[p], sems.at[1, 2 * i + k]))
    for load in loads:
        load.start()
    for load, store in zip(loads, stores):
        load.wait()
        store.start()
    for store in stores:
        store.wait()


def on_device(
    mixer_input,
    forget_cumsum,
    mixer_gain,
    query_weight,
    key_weight,
    value_weight,
    out_weight,
    post_gain,
    expert_input,
    expert_gain,
    routes,
    route_weight,
    expert_gate,
    expert_upward,
    expert_down,
):
    n_ep = lax.axis_size("ep")
    n_tp = lax.axis_size("tp")
    mix_rows, width = mixer_input.shape
    heads = forget_cumsum.shape[0]
    head_width = query_weight.shape[1]
    head_dim = head_width // heads
    span = mix_rows * n_tp
    moe_rows, top_count = routes.shape
    assert n_tp == 4 and expert_gate.shape[0] == 1
    capacity = (moe_rows * top_count * 9 + 8 * n_ep - 1) // (8 * n_ep)
    cap = (capacity + ROW_TILE - 1) // ROW_TILE * ROW_TILE
    f_width = expert_gate.shape[2]
    folded = n_ep == 4
    sets = 2 if folded else 1

    inputs = {
        "mixer_input": mixer_input,
        "mixer_gain": mixer_gain.reshape(1, -1),
        "routes": routes.T,
        "expert_input": expert_input,
        "expert_gain": expert_gain.reshape(1, -1),
        "wq": query_weight,
        "wk": key_weight,
        "wv": value_weight,
        "eg": expert_gate[0],
        "eu": expert_upward[0],
        "ed": expert_down[0],
        "route_weight": route_weight.T,
        "gate": forget_cumsum,
        "post_gain": post_gain.reshape(1, -1),
        "wo": out_weight,
    }
    vmem, dma = pltpu.VMEM, pltpu.SemaphoreType.DMA
    scratch = {name: vmem(x.shape, x.dtype) for name, x in inputs.items()}
    scratch |= {
        "seg": vmem((4, mix_rows, width), BF16),
        "queries": vmem((span, head_width), BF16),
        "kv": vmem((n_ep, span, 2 * head_width), BF16),
        "rows": vmem((n_ep, 4, cap, width), BF16),
        "out": vmem((n_ep, cap, width), BF16),
        "dispatch": vmem((n_ep, cap, moe_rows), BF16),
        "pick": vmem((n_ep, moe_rows, cap), BF16),
        "weights": vmem((moe_rows, LANES), F32),
        "combined": vmem((moe_rows, width), F32),
        "hid": vmem((2 * cap, f_width), BF16),
        "res": vmem((n_ep, 4, cap, width), BF16),
        "drec": vmem((n_ep, 2, cap, width), BF16),
        "erec": vmem((n_ep, cap, width), BF16),
        "ret": vmem((n_ep, cap, width), BF16),
        "run_max": vmem((sets, heads, span), F32),
        "run_sum": vmem((sets, heads, span), F32),
        "run_acc": vmem((sets, heads, head_dim, span), F32),
        "attended": vmem((span, head_width), BF16),
        "columns": vmem((3 if folded else 1, span, LANES), F32),
        "mdrec": vmem((2, mix_rows, width), BF16),
        "load_sem": dma((len(inputs),)),
    }
    if folded:
        scratch |= {
            "qin": vmem((span, head_width), BF16),
            "obuf": vmem((head_width, span), BF16),
            "lbuf": vmem((8, span), F32),
            "oin": vmem((head_width, span), BF16),
            "lin": vmem((8, span), F32),
            "qs": dma((1,)),
            "qr": dma((1,)),
            "os": dma((2,)),
            "or": dma((2,)),
        }
    scratch |= {"ns": dma((3,)), "nr": dma((3,)), "ms": dma((3,)), "mr": dma((3,))}
    for name in ("a", "c", "e", "f", "k"):
        scratch |= {name + "s": dma((n_ep,)), name + "r": dma((n_ep,))}
    for name in ("b", "d"):
        scratch |= {name + "s": dma((2, n_ep)), name + "r": dma((2, n_ep))}

    labels = [name + "_hbm" for name in inputs] + ["mixer_out", "expert_out"] + list(scratch)

    def body(*refs):
        kernel(n_ep, head_dim, dict(zip(labels, refs, strict=True)))

    block = pl.BlockSpec(memory_space=pltpu.VMEM)
    results = pl.pallas_call(
        body,
        out_shape=(
            jax.ShapeDtypeStruct((mix_rows, width), BF16),
            jax.ShapeDtypeStruct((moe_rows, width), BF16),
        ),
        in_specs=[pl.BlockSpec(memory_space=pl.ANY)] * len(inputs),
        out_specs=(block, block),
        scratch_shapes=list(scratch.values()),
        compiler_params=pltpu.CompilerParams(
            collective_id=0, has_side_effects=True, vmem_limit_bytes=66_500_000
        ),
    )(*inputs.values())
    anywhere = pl.BlockSpec(memory_space=pl.ANY)
    return pl.pallas_call(
        hand_out,
        out_shape=tuple(jax.ShapeDtypeStruct(x.shape, x.dtype) for x in results),
        in_specs=[anywhere] * 2,
        out_specs=(anywhere,) * 2,
        scratch_shapes=[vmem(x.shape, x.dtype) for x in results] + [dma((2, 4))],
    )(*results)


def solution(mesh):
    rows = P(("grp", "ep", "tp"), None)
    in_specs = (
        rows,
        P("tp", "grp"),
        P(),
        P(None, "tp"),
        P(None, "tp"),
        P(None, "tp"),
        P("tp", None),
        P(),
        rows,
        P(),
        rows,
        rows,
        P("ep", None, "tp"),
        P("ep", None, "tp"),
        P("ep", "tp", None),
    )
    return jax.shard_map(
        on_device, mesh=mesh, in_specs=in_specs, out_specs=(rows, rows), check_vma=False
    )
```
